512 devices in a mesh: ep: 32 (over z, core), tp: 16 (over y, x).
Axes of the slice: x: 4, y: 4, z: 16, core: 2. Of those that a mesh axis runs over, the one named last changes fastest.
Arguments:
- tokens: bfloat16 [512, 2048], P('ep'), may hold values from -6 to 6
- attn_gain: bfloat16 [2048], replicated, may hold values from 0.099609375 to 1.8984375
- w_query: bfloat16 [2048, 1024], P('ep', 'tp'), may hold values from -0.125 to 0.125
- w_key: bfloat16 [2048, 1024], P('ep', 'tp'), may hold values from -0.125 to 0.125
- w_value: bfloat16 [2048, 1024], P('ep', 'tp'), may hold values from -0.125 to 0.125
- w_forget: bfloat16 [2048, 16], P('ep', 'tp'), may hold values from -0.375 to 0.375
- forget_bias: float32 [16], P('tp'), may hold values from -2 to 2
- cache_keys: bfloat16 [512, 16, 1024, 64], P('ep', 'tp'), may hold values from -200 to 200
- cache_values: bfloat16 [512, 16, 1024, 64], P('ep', 'tp'), may hold values from -6 to 6
- cache_gates: float32 [512, 16, 1024], P('ep', 'tp'), may hold values from -256 to 0, as said below
- lengths: int32 [512], P('ep'), may hold values from 1 to 1024, 262144 in all
- w_out: bfloat16 [1024, 2048], P('tp', 'ep'), may hold values from -0.1875 to 0.1875
- moe_gain: bfloat16 [2048], replicated, may hold values from 0.099609375 to 1.8984375
- routing: int32 [512, 4], P('ep'), may hold values from 0 to 31, all different within a row; in each aligned block of 16 rows (0 to 15, 16 to 31, ...) at most 4 rows name the same one
- route_weight: float32 [512, 4], P('ep'), may hold values from 0.1 to 1
- w_gate: bfloat16 [32, 2048, 1024], P('ep', None, 'tp')
- w_up: bfloat16 [32, 2048, 1024], P('ep', None, 'tp')
- w_down: bfloat16 [32, 1024, 2048], P('ep', 'tp'), may hold values from -0.1875 to 0.1875
Outputs:
- layer_out: bfloat16 [512, 2048], P('ep')
The draws below stay inside these ranges and needn't reach their ends.
Inputs may be any that keep to these rules, and one draw needn't show every extreme that they name: `routing`: within the rows of one device (aligned blocks of 16 rows) no expert is named more than 4 times, a bound that some block reaches; each row names 4 different experts. lengths[s] is at least 1 and at most 1024; some sequence has exactly 1024. cache_gates[s, h, p] is the sum of the log forget gates of positions 0 to p of sequence s in head h; it never rises along p.
All inputs are finite; a program needn't handle non-finite values. No bound on the sum of `lengths` on one device may be relied on, other than what follows from the above.
Results may differ from the reference program's by a relative error of at most 0.012.
The reference program's roundings to bfloat16 on the way count: a program that leaves them out, or rounds other values in their place, can miss the bound.
Values may be sent and summed in bfloat16 or wider, within the bound.
No kernel may reach another device: no remote copies, remote signals or barrier semaphores. Data moves between devices by JAX's collectives and lax.ppermute only.
A program may use at most 64 MiB of HBM per device.

```python
import math
import jax
import jax.numpy as jnp
import numpy as np
from jax import lax

D = 2048
HEADS = 16
HD = 64
FF = 1024
TOPK = 4
SEQS = 16
CACHE = 1024
EXPERTS = 32
TOKENS = 512
CAP = 4
N_EP = 32


def draw_cache_keys(key, part):
    first = jax.random.fold_in(jax.random.fold_in(key, 11), 0)
    shape = (TOKENS, HEADS, CACHE, HD)
    return jnp.clip(jax.random.normal(first, shape, jnp.float32), -6.0, 6.0).astype(jnp.bfloat16)


def draw_cache_gates(key, part):
    keys_list = jax.random.split(jax.random.fold_in(key, 23), 6)
    slow_total = jnp.exp(jax.random.uniform(keys_list[0], (TOKENS, HEADS, 1), jnp.float32, jnp.log(0.5), jnp.log(2.0)))
    fast_rate = jnp.exp(jax.random.uniform(keys_list[1], (TOKENS, HEADS, 1), jnp.float32, jnp.log(0.01), jnp.log(1.0 / 30.0)))
    order = jax.random.permutation(keys_list[2], HEADS)
    fast_count = HEADS // 2
    is_fast = (order < fast_count)[None, :, None]
    base_rate = jnp.where(is_fast, fast_rate, slow_total / CACHE)
    seq_factor = jnp.exp(jax.random.uniform(keys_list[3], (TOKENS, 1, 1), jnp.float32, jnp.log(0.5), jnp.log(2.0)))
    spans = (CACHE + 15) // 16
    span_table = jnp.exp(jax.random.uniform(keys_list[4], (TOKENS, HEADS, spans), jnp.float32, -0.7, 0.7))
    span_factor = jnp.repeat(span_table, 16, axis=2)[:, :, :CACHE]
    noise = jax.random.uniform(keys_list[5], (TOKENS, HEADS, CACHE), jnp.float32, 0.5, 1.5)
    steps_taken = base_rate * seq_factor * span_factor * noise
    return -jnp.cumsum(steps_taken, axis=2)


def expert_weight_draw(key, salt):
    first = jax.random.fold_in(jax.random.fold_in(key, salt), 0)
    shape = (EXPERTS, D, FF)
    return (jnp.clip(jax.random.normal(first, shape, jnp.float32), -6.0, 6.0) * D ** (-0.5)).astype(jnp.bfloat16)


def draw_w_gate(key, part):
    return expert_weight_draw(key, 37)


def draw_w_up(key, part):
    return expert_weight_draw(key, 41)


def block_levels(own_key, dims, shards, low, high):
    level, own = 1.0, jax.random.fold_in(own_key, 6)
    for position, blocks in shards:
        heights = jnp.exp(jax.random.uniform(jax.random.fold_in(own, position), (blocks,), jnp.float32, low / len(shards), high / len(shards)))
        level = level * jnp.repeat(heights, dims[position] // blocks).reshape([-1 if axis == position else 1 for axis in range(len(dims))])
    return level


def profile(count, total, most, slope):
    weights = [(1 << 20) // math.isqrt(rank ** slope) + 1 for rank in range(2, count + 1)]
    rest, given = total - most - (count - 1), [1] * (count - 1)
    while rest > 0:
        free = [i for i in range(count - 1) if given[i] < most]
        pool, left = sum([weights[i] for i in free]), rest
        for i in free:
            addition = min(most - given[i], max(1, left * weights[i] // pool), rest)
            given[i] = given[i] + addition
            rest = rest - addition
    return np.array([most] + given)


def ragged_sizes(key, count, total, limit, slope):
    if count == 2:
        one = jax.random.randint(key, (), max(1, total - limit), min(limit, total - 1) + 1)
        return jnp.stack([one, total - one])
    sizes = jnp.asarray(profile(count, total, limit, slope), jnp.int32)
    pairs = (count - 1) // 2
    source_of, sink = sizes[1:1 + 2 * pairs:2], sizes[2:2 + 2 * pairs:2]
    slack = jnp.minimum(source_of - 1, limit - sink)
    moved = jax.random.randint(jax.random.fold_in(key, 1), (pairs,), 0, 1 << 20) % (slack + 1)
    sizes = sizes.at[1:1 + 2 * pairs:2].set(source_of - moved).at[2:2 + 2 * pairs:2].set(sink + moved)
    return sizes[jax.random.permutation(jax.random.fold_in(key, 2), count)]


def assign_block(rng, own, number, rows, amount, top, bound, skew):
    sequence = jax.random.permutation(rng, amount)
    crowded, ordinary = shares(amount, rows * top, bound, skew, True), shares(amount, rows * top, bound, skew, False)
    places = jnp.arange(amount)

    def named(sizes, rotation):
        used = int((sizes > 0).sum())
        fixed = max(1, used // 4)
        moved = fixed + (places - fixed + rotation * (used - fixed)) % max(1, amount - fixed)
        return jnp.zeros((amount,), jnp.int32).at[sequence[jnp.where(places < fixed, places, moved)]].set(jnp.asarray(sizes, jnp.int32))

    sizes = jnp.where(number % 4 == 0, named(crowded, number // 4), named(ordinary, number - number // 4 - 1))
    mixed = jax.random.permutation(jax.random.fold_in(own, 3), amount)
    source_of, taker = mixed[0:amount // 2 * 2:2], mixed[1:amount // 2 * 2:2]
    slack = jnp.minimum(sizes[source_of] - 1, bound - sizes[taker]) // 2
    slack = jnp.where((source_of == sequence[0]) | (taker == sequence[0]) | (sizes[taker] == 0), 0, jnp.maximum(slack, 0))
    moved = jax.random.randint(jax.random.fold_in(own, 4), (amount // 2,), 0, 1 << 20) % (slack + 1)
    sizes = sizes.at[source_of].add(-moved).at[taker].add(moved)
    members = jnp.searchsorted(jnp.cumsum(sizes), jnp.arange(rows * top), side="right").astype(jnp.int32)
    grid = members.reshape(top, rows).T
    grid = grid[jax.random.permutation(jax.random.fold_in(own, 1), rows)]
    rotation = jax.random.randint(jax.random.fold_in(own, 2), (rows, 1), 0, top)
    return jnp.take_along_axis(grid, (jnp.arange(top)[None, :] + rotation) % top, axis=1)


def shares(number_of, total, bound, skew, full):
    loads = [(1 << 20) // math.isqrt(standing ** skew) + 1 for standing in range(1, number_of + 1)]
    largest = bound if full else min(bound, max(-(-total // number_of), total * loads[0] // sum(loads)))
    least = 1 if total - largest >= number_of - 1 else 0
    given, rest = [largest] + [least] * (number_of - 1), total - largest - least * (number_of - 1)
    while rest > 0:
        free = [i for i in range(1, number_of) if given[i] < largest] or [i for i in range(1, number_of) if given[i] < bound]
        mass, left = sum([loads[i] for i in free]), rest
        for i in free:
            more = min(bound - given[i], max(1, left * loads[i] // mass), rest)
            given[i] = given[i] + more
            rest = rest - more
    return np.array(given)


def scatter_about(stream_key, shape, scale, limit, cuts=(), kind=jnp.bfloat16):
    entries = scale * jax.random.normal(stream_key, shape, jnp.float32)
    if cuts:
        entries = entries * block_levels(stream_key, shape, cuts, -0.22, 0.18)
    return jnp.clip(entries, -limit, limit).astype(kind)


def setup_inputs(seed: int = 0) -> dict:
    key_of = jax.random.split(jax.random.key(seed), 19)
    tokens = scatter_about(key_of[0], (TOKENS, D), 1.0, 6.0, ((0, 32),))
    attn_gain = jnp.clip(1.0 + 0.18 * jax.random.normal(key_of[1], (D,), jnp.float32), 0.099609375, 1.8984375).astype(jnp.bfloat16)
    w_query = scatter_about(key_of[2], (D, HEADS * HD), D ** -0.5, 0.125, ((0, 32), (1, 16)))
    w_key = scatter_about(key_of[3], (D, HEADS * HD), D ** -0.5, 0.125, ((0, 32), (1, 16)))
    w_value = scatter_about(key_of[4], (D, HEADS * HD), D ** -0.5, 0.125, ((0, 32), (1, 16)))
    w_forget = scatter_about(key_of[5], (D, HEADS), (D // 9) ** -0.5, 0.375, ((0, 32), (1, 16)))
    forget_bias = jnp.clip(jax.random.uniform(key_of[6], (HEADS,), jnp.float32, -2.0, 2.0) * block_levels(key_of[6], (HEADS,), ((0, 16),), -0.4, 0.0), -2.0, 2.0)
    cache_keys = draw_cache_keys(jax.random.fold_in(key_of[18], 71), 0)
    cache_values = scatter_about(key_of[8], (TOKENS, HEADS, CACHE, HD), 1.0, 6.0, ((0, 32), (1, 16)))
    cache_gates = draw_cache_gates(jax.random.fold_in(key_of[18], 71), 0)
    lengths = ragged_sizes(key_of[10], TOKENS, TOKENS * CACHE // 2, CACHE, 2).astype(jnp.int32)
    w_out = scatter_about(key_of[11], (HEADS * HD, D), (HEADS * HD) ** -0.5, 0.1875, ((0, 16), (1, 32)))
    moe_gain = jnp.clip(1.0 + 0.18 * jax.random.normal(key_of[12], (D,), jnp.float32), 0.099609375, 1.8984375).astype(jnp.bfloat16)
    routing_keys = jax.random.split(jax.random.fold_in(key_of[13], 1), TOKENS // SEQS)
    routing_turns = jax.random.permutation(jax.random.fold_in(key_of[13], 3), TOKENS // SEQS)
    routing = jax.vmap(lambda own, number: assign_block(jax.random.fold_in(key_of[13], 2), own, number, SEQS, EXPERTS, TOPK, CAP, 2))(routing_keys, routing_turns).reshape((TOKENS, TOPK))
    route_weight = jnp.clip(jnp.exp(math.log(1.0) - 2.3025851 * jax.random.uniform(key_of[14], (TOKENS, TOPK), jnp.float32) ** block_levels(key_of[14], (TOKENS, TOPK), ((0, 32),), -0.2, 0.2)), 0.1, 1.0)
    w_gate = draw_w_gate(jax.random.fold_in(key_of[18], 71), 0)
    w_up = draw_w_up(jax.random.fold_in(key_of[18], 71), 0)
    w_down = scatter_about(key_of[17], (EXPERTS, FF, D), FF ** -0.5, 0.1875, ((0, 32), (1, 16)))
    return {"tokens": tokens, "attn_gain": attn_gain, "w_query": w_query, "w_key": w_key, "w_value": w_value, "w_forget": w_forget, "forget_bias": forget_bias, "cache_keys": cache_keys, "cache_values": cache_values, "cache_gates": cache_gates, "lengths": lengths, "w_out": w_out, "moe_gain": moe_gain, "routing": routing, "route_weight": route_weight, "w_gate": w_gate, "w_up": w_up, "w_down": w_down}


NORM_EPSILON = 1e-06
CLAMP_LIMIT = 7.0
SIGMOID_SLOPE = 1.702

def rms_norm(values, gain_vector):
    widened = values.astype(jnp.float32)
    scaled = widened * lax.rsqrt(lax.optimization_barrier(jnp.mean(widened * widened, axis=-1, keepdims=True)) + NORM_EPSILON)
    return (scaled * gain_vector.astype(jnp.float32)).astype(jnp.bfloat16)

def attend(inputs):
    query, key_new, value_new, log_gate, keys_cached, values_cached, gates_cached, lengths_here = inputs
    head_size = query.shape[-1]
    scale = head_size ** (-0.5)
    positions = jnp.arange(keys_cached.shape[2], dtype=jnp.int32)
    valid = positions[None, None, :] < lengths_here[:, None, None]
    is_last = positions[None, None, :] == lengths_here[:, None, None] - 1
    last_gate = lax.optimization_barrier(jnp.sum(jnp.where(is_last, gates_cached, jnp.float32(0.0)), axis=-1))
    new_gate = last_gate + log_gate
    query_wide = query.astype(jnp.float32)
    scores = jnp.einsum('shd,shld->shl', query_wide, keys_cached.astype(jnp.float32)) * scale
    scores = scores + (new_gate[..., None] - gates_cached)
    scores = jnp.where(valid, scores, -jnp.inf)
    own_score = lax.optimization_barrier(jnp.sum(query_wide * key_new.astype(jnp.float32), axis=-1)) * scale
    highest = jnp.maximum(lax.optimization_barrier(jnp.max(scores, axis=-1)), own_score)
    cached_weight = jnp.exp(scores - highest[..., None])
    own_weight = jnp.exp(own_score - highest)
    denominator = lax.optimization_barrier(jnp.sum(cached_weight, axis=-1)) + own_weight
    cached_share = (cached_weight / denominator[..., None]).astype(jnp.bfloat16)
    attended = jnp.einsum('shl,shld->shd', cached_share.astype(jnp.float32), values_cached.astype(jnp.float32))
    attended = attended + (own_weight / denominator)[..., None] * value_new.astype(jnp.float32)
    return attended.astype(jnp.bfloat16)

def expert_partial(token_rows, gate_matrix, up_matrix, down_matrix):
    gate_pre = jnp.dot(token_rows, gate_matrix, preferred_element_type=jnp.float32)
    up_pre = jnp.dot(token_rows, up_matrix, preferred_element_type=jnp.float32)
    gate_cut = jnp.minimum(gate_pre, CLAMP_LIMIT)
    up_cut = jnp.clip(up_pre, -CLAMP_LIMIT, CLAMP_LIMIT)
    hidden = ((up_cut + 1.0) * gate_cut * jax.nn.sigmoid(SIGMOID_SLOPE * gate_cut)).astype(jnp.bfloat16)
    return jnp.dot(hidden, down_matrix, preferred_element_type=jnp.float32)

def reference(tokens, attn_gain, w_query, w_key, w_value, w_forget, forget_bias, cache_keys, cache_values, cache_gates, lengths, w_out, moe_gain, routing, route_weight, w_gate, w_up, w_down):
    normed = rms_norm(tokens, attn_gain)
    query = jnp.dot(normed, w_query, preferred_element_type=jnp.float32).astype(jnp.bfloat16)
    key_new = jnp.dot(normed, w_key, preferred_element_type=jnp.float32).astype(jnp.bfloat16)
    value_new = jnp.dot(normed, w_value, preferred_element_type=jnp.float32).astype(jnp.bfloat16)
    forget_pre = jnp.dot(normed, w_forget, preferred_element_type=jnp.float32)
    log_gate = jax.nn.log_sigmoid(forget_pre + forget_bias)
    attended = lax.map(attend, (query.reshape(N_EP, SEQS, HEADS, HD), key_new.reshape(N_EP, SEQS, HEADS, HD), value_new.reshape(N_EP, SEQS, HEADS, HD), log_gate.reshape(N_EP, SEQS, HEADS), cache_keys.reshape(N_EP, SEQS, HEADS, CACHE, HD), cache_values.reshape(N_EP, SEQS, HEADS, CACHE, HD), cache_gates.reshape(N_EP, SEQS, HEADS, CACHE), lengths.reshape(N_EP, SEQS)))
    attended = attended.reshape(TOKENS, HEADS * HD)
    residual = tokens.astype(jnp.float32) + jnp.dot(attended, w_out, preferred_element_type=jnp.float32)
    normed_two = rms_norm(residual, moe_gain)
    flat = routing.reshape(N_EP, SEQS * TOPK)
    onehot = (flat[..., None] == jnp.arange(EXPERTS, dtype=jnp.int32)).astype(jnp.int32)
    earlier = jnp.cumsum(onehot, axis=1) - onehot
    slot_index = lax.optimization_barrier(jnp.sum(earlier * onehot, axis=-1)).astype(jnp.int32)
    source = jnp.broadcast_to(jnp.arange(N_EP, dtype=jnp.int32)[:, None], flat.shape)
    repeated = jnp.repeat(normed_two, TOPK, axis=0).reshape(N_EP, SEQS * TOPK, D)
    buffers = jnp.zeros((EXPERTS, N_EP, CAP, D), jnp.bfloat16).at[flat, source, slot_index].set(repeated)

    def run_expert(inputs):
        buffer_rows, gate_matrix, up_matrix, down_matrix = inputs
        summed = expert_partial(buffer_rows.reshape(N_EP * CAP, D), gate_matrix, up_matrix, down_matrix)
        return summed.astype(jnp.bfloat16).reshape(N_EP, CAP, D)
    outputs = lax.map(run_expert, (buffers, w_gate, w_up, w_down))
    picked = outputs[flat, source, slot_index].astype(jnp.float32).reshape(TOKENS, TOPK, D)
    expert_sum = lax.optimization_barrier(jnp.sum(route_weight[..., None] * picked, axis=1))
    return (residual + expert_sum).astype(jnp.bfloat16)
```

```python
import jax
import jax.numpy as jnp
from jax import lax
from jax.sharding import PartitionSpec as P

NORM_EPSILON = 1e-06
CLAMP_LIMIT = 7.0
SIGMOID_SLOPE = 1.702
F32 = jnp.float32
BF16 = jnp.bfloat16


def to_everyone(shard, axis):
    size = lax.axis_size(axis)
    return lax.all_to_all(
        jnp.broadcast_to(shard[None], (size, *shard.shape)), axis, 0, 0, tiled=True
    )


def local(
    tokens,
    attn_gain,
    w_query,
    w_key,
    w_value,
    w_forget,
    forget_bias,
    cache_keys,
    cache_values,
    cache_gates,
    lengths,
    w_out,
    moe_gain,
    routing,
    route_weight,
    w_gate,
    w_up,
    w_down,
):
    n_ep = lax.axis_size("ep")
    n_tp = lax.axis_size("tp")
    rows, width = tokens.shape
    head = cache_keys.shape[3]
    chips = n_ep // 2
    block = width // n_ep
    narrow = width // n_tp
    core = lax.axis_index("ep") % 2
    offset = lax.axis_index("tp") * narrow

    packed = jnp.concatenate([w_query, w_key, w_value, w_out.T, w_forget], axis=1)
    same_core = [[2 * z + c for z in range(chips)] for c in range(2)]
    mine = lax.all_gather(packed, "ep", axis=0, tiled=True, axis_index_groups=same_core)
    theirs = lax.ppermute(mine, "ep", [(i, i ^ 1) for i in range(n_ep)])

    wide = tokens.astype(F32)
    normed = wide * lax.rsqrt(jnp.mean(wide * wide, axis=-1, keepdims=True) + NORM_EPSILON)
    normed = (normed * attn_gain.astype(F32)).astype(BF16)
    by_core = normed.reshape(rows, chips, 2, block)
    even = by_core[:, :, 0].reshape(rows, chips * block)
    odd = by_core[:, :, 1].reshape(rows, chips * block)
    is_odd = core == 1
    first = jnp.where(is_odd, theirs, mine)
    second = jnp.where(is_odd, mine, theirs)
    projected = jnp.dot(even, first, preferred_element_type=F32) + jnp.dot(
        odd, second, preferred_element_type=F32
    )
    query = projected[:, :head].astype(BF16)
    key_new = projected[:, head : 2 * head].astype(BF16)
    value_new = projected[:, 2 * head : 3 * head].astype(BF16)
    log_gate = jax.nn.log_sigmoid(projected[:, 4 * head] + forget_bias[0])

    keys = cache_keys[:, 0]
    values = cache_values[:, 0]
    gates = cache_gates[:, 0]
    scale = head ** (-0.5)
    positions = jnp.arange(keys.shape[1], dtype=jnp.int32)
    valid = positions[None, :] < lengths[:, None]
    is_last = positions[None, :] == lengths[:, None] - 1
    last_gate = jnp.sum(jnp.where(is_last, gates, F32(0.0)), axis=-1)
    new_gate = last_gate + log_gate
    scores = jnp.einsum("sd,sld->sl", query, keys, preferred_element_type=F32) * scale
    scores = scores + (new_gate[:, None] - gates)
    scores = jnp.where(valid, scores, -jnp.inf)
    own_score = jnp.sum(query.astype(F32) * key_new.astype(F32), axis=-1) * scale
    highest = jnp.maximum(jnp.max(scores, axis=-1), own_score)
    cached_weight = jnp.exp(scores - highest[:, None])
    own_weight = jnp.exp(own_score - highest)
    denominator = jnp.sum(cached_weight, axis=-1) + own_weight
    share = (cached_weight / denominator[:, None]).astype(BF16)
    attended = jnp.einsum("sl,sld->sd", share, values, preferred_element_type=F32)
    attended = attended + (own_weight / denominator)[:, None] * value_new.astype(F32)
    attended = attended.astype(BF16)

    out_first = first[:, 3 * head : 4 * head].reshape(chips, block, head)
    out_second = second[:, 3 * head : 4 * head].reshape(chips, block, head)
    out_blocks = jnp.concatenate([out_first, out_second], axis=1)
    head_terms = jnp.einsum("sd,zfd->zsf", attended, out_blocks, preferred_element_type=F32)
    parts = lax.all_to_all(head_terms, "tp", 0, 0, tiled=True)
    residual = lax.dynamic_slice_in_dim(tokens, offset, narrow, 1).astype(F32) + jnp.sum(parts, axis=0)

    top = routing.shape[1]
    capacity = max(1, 2 * rows * top // n_ep)
    flat = routing.reshape(-1)
    order = jnp.arange(rows * top, dtype=jnp.int32)
    same = (flat[:, None] == flat[None, :]) & (order[None, :] < order[:, None])
    target = flat * capacity + jnp.sum(same.astype(jnp.int32), axis=1)
    slots = n_ep * capacity
    hits = jnp.arange(slots, dtype=jnp.int32)[:, None, None] == target.reshape(rows, top)[None]
    selector = jnp.any(hits, axis=2).astype(BF16)
    mix = jnp.sum(jnp.where(hits, route_weight[None], F32(0.0)), axis=2)

    gain_here = lax.dynamic_slice_in_dim(moe_gain, offset, narrow, 0).astype(F32)
    scaled = (residual * gain_here).astype(BF16)
    squares = jnp.sum(residual * residual, axis=1)
    high = squares.astype(BF16)
    low = (squares - high.astype(F32)).astype(BF16)
    lane = jnp.arange(narrow, dtype=jnp.int32)[None, :]
    marks = jnp.where(lane == 0, high[:, None], jnp.where(lane == 1, low[:, None], BF16(0)))
    chosen = jnp.dot(selector, jnp.concatenate([scaled, marks], axis=1), preferred_element_type=F32)
    chosen = chosen.astype(BF16)
    sent = jnp.concatenate(
        [
            chosen[:, :narrow].reshape(n_ep, capacity, narrow),
            chosen[:, narrow:].reshape(n_ep, capacity, narrow),
        ],
        axis=1,
    )
    received = lax.all_to_all(sent, "ep", 0, 0, tiled=True)
    slices = received[:, :capacity].reshape(slots, narrow)
    marks_in = received[:, capacity:, :2].reshape(slots, 2)
    marks_rows = jnp.pad(marks_in.T, ((0, 14), (0, narrow - slots))) if slots <= narrow else None
    gathered = to_everyone(jnp.concatenate([slices, marks_rows], axis=0), "tp")
    full = gathered[:, :slots]
    total = jnp.sum(gathered[:, slots : slots + 2, :slots].astype(F32), axis=(0, 1))
    row_scale = lax.rsqrt(total / width + NORM_EPSILON)

    gate_pre = jnp.einsum(
        "trf,tfu->ru", full, w_gate[0].reshape(n_tp, narrow, -1), preferred_element_type=F32
    ) * row_scale[:, None]
    up_pre = jnp.einsum(
        "trf,tfu->ru", full, w_up[0].reshape(n_tp, narrow, -1), preferred_element_type=F32
    ) * row_scale[:, None]
    gate_cut = jnp.minimum(gate_pre, CLAMP_LIMIT)
    up_cut = jnp.clip(up_pre, -CLAMP_LIMIT, CLAMP_LIMIT)
    hidden = ((up_cut + 1.0) * gate_cut * jax.nn.sigmoid(SIGMOID_SLOPE * gate_cut)).astype(BF16)
    down = w_down[0].reshape(-1, n_tp, narrow)
    partial = jnp.einsum("ru,utf->trf", hidden, down, preferred_element_type=F32).astype(BF16)
    partial = lax.all_to_all(partial, "tp", 0, 0, tiled=True)
    served = jnp.sum(partial.astype(F32), axis=0).astype(BF16)

    returned = lax.all_to_all(served.reshape(n_ep, capacity, narrow), "ep", 0, 0, tiled=True)
    expert_sum = lax.dot_general(
        mix,
        returned.reshape(slots, narrow).astype(F32),
        (((0,), (0,)), ((), ())),
        precision=lax.Precision.HIGHEST,
        preferred_element_type=F32,
    )
    out_part = (residual + expert_sum).astype(BF16)
    final = to_everyone(out_part, "tp")
    return jnp.moveaxis(final, 0, 1).reshape(rows, width)


def solution(mesh):
    in_specs = (
        P("ep", None),
        P(),
        P("ep", "tp"),
        P("ep", "tp"),
        P("ep", "tp"),
        P("ep", "tp"),
        P("tp"),
        P("ep", "tp", None, None),
        P("ep", "tp", None, None),
        P("ep", "tp", None),
        P("ep"),
        P("tp", "ep"),
        P(),
        P("ep", None),
        P("ep", None),
        P("ep", None, "tp"),
        P("ep", None, "tp"),
        P("ep", "tp", None),
    )
    out_specs = P("ep", None)
    return jax.shard_map(local, mesh=mesh, in_specs=in_specs, out_specs=out_specs, check_vma=False)
```

```python
import jax
import jax.numpy as jnp
from jax import lax
from jax.experimental import pallas as pl
from jax.experimental.pallas import tpu as pltpu
from jax.sharding import PartitionSpec as P

NORM_EPSILON = 1e-06
CLAMP_LIMIT = 7.0
SIGMOID_SLOPE = 1.702
F32 = jnp.float32
BF16 = jnp.bfloat16


def to_everyone(shard, axis):
    size = lax.axis_size(axis)
    return lax.all_to_all(
        jnp.broadcast_to(shard[None], (size, *shard.shape)), axis, 0, 0, tiled=True
    )


PACK_ROWS = 72


def attention_kernel(
    core_ref, lengths_ref, bias_ref, tokens_ref, gain_ref, mine_ref, theirs_ref, gates_ref, keys_hbm, values_hbm,
    out_ref, keys_ref, values_ref, sems,
):
    rows, width = tokens_ref.shape
    cached = keys_ref.shape[1]
    head = keys_ref.shape[0] // rows
    chips = mine_ref.shape[0]
    key_copy = pltpu.make_async_copy(keys_hbm, keys_ref, sems.at[0])
    value_copy = pltpu.make_async_copy(values_hbm, values_ref, sems.at[1])
    key_copy.start()
    value_copy.start()

    wide = tokens_ref[...].astype(F32)
    scale_row = lax.rsqrt(jnp.mean(wide * wide, axis=-1, keepdims=True) + NORM_EPSILON)
    normed = (wide * scale_row * gain_ref[...].astype(F32)).astype(BF16)

    is_odd = core_ref[0] == 1
    projected = jnp.zeros((rows, 256), F32)
    shifted = jnp.zeros((rows, 128), F32)
    forget = jnp.zeros((rows, 128), F32)
    out_tiles = []
    for z in range(chips):
        own = mine_ref[z]
        other = theirs_ref[z]
        first = jnp.where(is_odd, other, own)
        second = jnp.where(is_odd, own, other)
        left = normed[:, z * 128 : (z + 1) * 128]
        stacked = jnp.concatenate([first[:64, :128], second[:64, :128]], axis=0)
        projected_qk = jnp.dot(left, stacked, preferred_element_type=F32)
        both = jnp.concatenate([first[:64, 128:], second[:64, 128:]], axis=0)
        lane = lax.broadcasted_iota(jnp.int32, left.shape, 1)
        even_left = jnp.where(lane < 64, left, jnp.zeros_like(left))
        odd_left = jnp.where(lane < 64, jnp.zeros_like(left), left)
        projected = projected + jnp.concatenate(
            [projected_qk, jnp.dot(odd_left, both, preferred_element_type=F32)], axis=1
        )
        shifted = shifted + jnp.dot(even_left, both, preferred_element_type=F32)
        out_tiles.append((first[:64, 128:], second[:64, 128:]))
        weights = jnp.concatenate([first[64:65, :64], second[64:65, :64]], axis=1)
        forget = forget + left.astype(F32) * weights.astype(F32)
    query = projected[:, :head].astype(BF16)
    key_new = projected[:, head : 2 * head].astype(BF16)
    value_new = (projected[:, 2 * head : 3 * head] + shifted[:, head:]).astype(BF16)
    forget_pre = jnp.sum(forget, axis=1, keepdims=True) + bias_ref[0]
    log_gate = jnp.minimum(forget_pre, 0.0) - jnp.log1p(jnp.exp(-jnp.abs(forget_pre)))

    gates = gates_ref[...].reshape(rows, cached)
    row = lax.broadcasted_iota(jnp.int32, (rows, 1), 0)
    count = jnp.zeros((rows, 1), jnp.int32)
    for s in range(rows):
        count = jnp.where(row == s, lengths_ref[s], count)
    position = lax.broadcasted_iota(jnp.int32, (rows, cached), 1)
    last_gate = jnp.sum(jnp.where(position == count - 1, gates, 0.0), axis=-1, keepdims=True)
    new_gate = last_gate + log_gate

    owner = lax.broadcasted_iota(jnp.int32, (rows, rows * head), 1) // head
    diagonal = owner == lax.broadcasted_iota(jnp.int32, (rows, rows * head), 0)
    repeated = jnp.concatenate([query] * rows, axis=1)
    spread = jnp.where(diagonal, repeated, jnp.zeros_like(repeated))
    scale = head ** (-0.5)
    key_copy.wait()
    scores = jnp.dot(spread, keys_ref[...], preferred_element_type=F32) * scale
    scores = scores + (new_gate - gates)
    scores = jnp.where(position < count, scores, -jnp.inf)
    own_score = jnp.sum(query.astype(F32) * key_new.astype(F32), axis=-1, keepdims=True) * scale
    highest = jnp.maximum(jnp.max(scores, axis=-1, keepdims=True), own_score)
    cached_weight = jnp.exp(scores - highest)
    own_weight = jnp.exp(own_score - highest)
    denominator = jnp.sum(cached_weight, axis=-1, keepdims=True) + own_weight
    share = (cached_weight / denominator).astype(BF16)
    value_copy.wait()
    crossed = lax.dot_general(
        share, values_ref[...], (((1,), (1,)), ((), ())), preferred_element_type=F32
    )
    crossed = jnp.where(diagonal, crossed, 0.0)
    folded = crossed[:, :128]
    for b in range(1, rows * head // 128):
        folded = folded + crossed[:, b * 128 : (b + 1) * 128]
    attended = folded[:, :head] + folded[:, head:]
    attended = attended + (own_weight / denominator) * value_new.astype(F32)
    attended = attended.astype(BF16)
    lane = lax.broadcasted_iota(jnp.int32, (rows, 128), 1)
    for z in range(chips):
        first, second = out_tiles[z]
        low = jnp.dot(attended, first, preferred_element_type=F32)
        high = jnp.dot(attended, second, preferred_element_type=F32)
        out_ref[z] = jnp.where(lane < head, low, high)


def local(
    tokens,
    attn_gain,
    w_query,
    w_key,
    w_value,
    w_forget,
    forget_bias,
    cache_keys,
    cache_values,
    cache_gates,
    lengths,
    w_out,
    moe_gain,
    routing,
    route_weight,
    w_gate,
    w_up,
    w_down,
):
    n_ep = lax.axis_size("ep")
    n_tp = lax.axis_size("tp")
    rows, width = tokens.shape
    head = cache_keys.shape[3]
    chips = n_ep // 2
    block = width // n_ep
    narrow = width // n_tp
    core = lax.axis_index("ep") % 2
    offset = lax.axis_index("tp") * narrow

    is_odd = core == 1
    packed = jnp.concatenate(
        [w_query, w_key, jnp.where(is_odd, w_value, w_out), jnp.where(is_odd, w_out, w_value)], axis=1
    )
    extra = jnp.pad(w_forget.T, ((0, PACK_ROWS - block - 1), (0, packed.shape[1] - block)))
    packed = jnp.concatenate([packed, extra], axis=0)
    same_core = [[2 * z + c for z in range(chips)] for c in range(2)]
    mine = lax.all_gather(packed, "ep", axis=0, tiled=False, axis_index_groups=same_core)
    theirs = lax.ppermute(mine, "ep", [(i, i ^ 1) for i in range(n_ep)])

    cached = cache_keys.shape[2]
    smem = pl.BlockSpec(memory_space=pltpu.SMEM)
    vmem = pl.BlockSpec(memory_space=pltpu.VMEM)
    anywhere = pl.BlockSpec(memory_space=pl.ANY)
    head_terms = pl.pallas_call(
        attention_kernel,
        out_shape=jax.ShapeDtypeStruct((n_tp, rows, narrow), F32),
        in_specs=[smem, smem, smem, vmem, vmem, vmem, vmem, vmem, anywhere, anywhere],
        out_specs=vmem,
        scratch_shapes=[
            pltpu.VMEM((rows * head, cached), BF16),
            pltpu.VMEM((rows * head, cached), BF16),
            pltpu.SemaphoreType.DMA((2,)),
        ],
        name="attention",
    )(
        core.reshape(1),
        lengths,
        forget_bias,
        tokens,
        attn_gain.reshape(1, width),
        mine,
        theirs,
        cache_gates,
        jnp.swapaxes(cache_keys[:, 0], 1, 2).reshape(rows * head, cached),
        jnp.swapaxes(cache_values[:, 0], 1, 2).reshape(rows * head, cached),
    )
    parts = lax.all_to_all(head_terms, "tp", 0, 0, tiled=True)
    residual = lax.dynamic_slice_in_dim(tokens, offset, narrow, 1).astype(F32) + jnp.sum(parts, axis=0)

    top = routing.shape[1]
    capacity = max(1, 2 * rows * top // n_ep)
    flat = routing.reshape(-1)
    order = jnp.arange(rows * top, dtype=jnp.int32)
    same = (flat[:, None] == flat[None, :]) & (order[None, :] < order[:, None])
    target = flat * capacity + jnp.sum(same.astype(jnp.int32), axis=1)
    slots = n_ep * capacity
    hits = jnp.arange(slots, dtype=jnp.int32)[:, None, None] == target.reshape(rows, top)[None]
    selector = jnp.any(hits, axis=2).astype(BF16)
    mix = jnp.sum(jnp.where(hits, route_weight[None], F32(0.0)), axis=2)

    gain_here = lax.dynamic_slice_in_dim(moe_gain, offset, narrow, 0).astype(F32)
    scaled = (residual * gain_here).astype(BF16)
    squares = jnp.sum(residual * residual, axis=1)
    high = squares.astype(BF16)
    low = (squares - high.astype(F32)).astype(BF16)
    lane = jnp.arange(narrow, dtype=jnp.int32)[None, :]
    marks = jnp.where(lane == 0, high[:, None], jnp.where(lane == 1, low[:, None], BF16(0)))
    chosen = jnp.dot(selector, jnp.concatenate([scaled, marks], axis=1), preferred_element_type=F32)
    chosen = chosen.astype(BF16)
    sent = jnp.concatenate(
        [
            chosen[:, :narrow].reshape(n_ep, capacity, narrow),
            chosen[:, narrow:].reshape(n_ep, capacity, narrow),
        ],
        axis=1,
    )
    received = lax.all_to_all(sent, "ep", 0, 0, tiled=True)
    slices = received[:, :capacity].reshape(slots, narrow)
    marks_in = received[:, capacity:, :2].reshape(slots, 2)
    marks_rows = jnp.pad(marks_in.T, ((0, 14), (0, narrow - slots))) if slots <= narrow else None
    gathered = to_everyone(jnp.concatenate([slices, marks_rows], axis=0), "tp")
    full = gathered[:, :slots]
    total = jnp.sum(gathered[:, slots : slots + 2, :slots].astype(F32), axis=(0, 1))
    row_scale = lax.rsqrt(total / width + NORM_EPSILON)

    gate_pre = jnp.einsum(
        "trf,tfu->ru", full, w_gate[0].reshape(n_tp, narrow, -1), preferred_element_type=F32
    ) * row_scale[:, None]
    up_pre = jnp.einsum(
        "trf,tfu->ru", full, w_up[0].reshape(n_tp, narrow, -1), preferred_element_type=F32
    ) * row_scale[:, None]
    gate_cut = jnp.minimum(gate_pre, CLAMP_LIMIT)
    up_cut = jnp.clip(up_pre, -CLAMP_LIMIT, CLAMP_LIMIT)
    hidden = ((up_cut + 1.0) * gate_cut * jax.nn.sigmoid(SIGMOID_SLOPE * gate_cut)).astype(BF16)
    down = w_down[0].reshape(-1, n_tp, narrow)
    partial = jnp.einsum("ru,utf->trf", hidden, down, preferred_element_type=F32).astype(BF16)
    partial = lax.all_to_all(partial, "tp", 0, 0, tiled=True)
    served = jnp.sum(partial.astype(F32), axis=0).astype(BF16)

    returned = lax.all_to_all(served.reshape(n_ep, capacity, narrow), "ep", 0, 0, tiled=True)
    expert_sum = lax.dot_general(
        mix,
        returned.reshape(slots, narrow).astype(F32),
        (((0,), (0,)), ((), ())),
        precision=lax.Precision.HIGHEST,
        preferred_element_type=F32,
    )
    out_part = (residual + expert_sum).astype(BF16)
    final = to_everyone(out_part, "tp")
    return jnp.moveaxis(final, 0, 1).reshape(rows, width)


def solution(mesh):
    in_specs = (
        P("ep", None),
        P(),
        P("ep", "tp"),
        P("ep", "tp"),
        P("ep", "tp"),
        P("ep", "tp"),
        P("tp"),
        P("ep", "tp", None, None),
        P("ep", "tp", None, None),
        P("ep", "tp", None),
        P("ep"),
        P("tp", "ep"),
        P(),
        P("ep", None),
        P("ep", None),
        P("ep", None, "tp"),
        P("ep", None, "tp"),
        P("ep", "tp", None),
    )
    out_specs = P("ep", None)
    return jax.shard_map(local, mesh=mesh, in_specs=in_specs, out_specs=out_specs, check_vma=False)
```

```python
import jax
import jax.numpy as jnp
from jax import lax
from jax.experimental import pallas as pl
from jax.experimental.pallas import tpu as pltpu
from jax.sharding import PartitionSpec as P

NORM_EPSILON = 1e-06
CLAMP_LIMIT = 7.0
SIGMOID_SLOPE = 1.702
F32 = jnp.float32
BF16 = jnp.bfloat16


def to_everyone(shard, axis):
    size = lax.axis_size(axis)
    return lax.all_to_all(
        jnp.broadcast_to(shard[None], (size, *shard.shape)), axis, 0, 0, tiled=True
    )


PACK_ROWS = 72
LIMIT = 16 * 2**20
CAPACITY = 4


def settle_kernel(packed_ref, out_ref):
    out_ref[...] = packed_ref[...]


def prepare_kernel(
    core_ref, place_ref, mine_ref, tokens_ref, gain_ref, moe_gain_ref, routing_ref, weight_ref,
    normed_ref, sums_ref, slice_ref, moe_slice_ref, choice_ref, mix_ref,
):
    rows, width = tokens_ref.shape
    narrow = slice_ref.shape[1]
    tokens = tokens_ref[...]
    wide = tokens.astype(F32)
    scale_row = lax.rsqrt(jnp.mean(wide * wide, axis=-1, keepdims=True) + NORM_EPSILON)
    normed = (wide * scale_row * gain_ref[...].astype(F32).reshape(1, width)).astype(BF16)
    normed_ref[...] = normed
    sums_ref[...] = half_sums(normed, mine_ref, core_ref[0], rows)

    place = place_ref[0]
    moe_gain = moe_gain_ref[...].astype(F32).reshape(1, width)
    part = jnp.zeros((rows, narrow), F32)
    moe_part = jnp.zeros((1, narrow), F32)
    for t in range(width // narrow):
        part = jnp.where(place == t, wide[:, t * narrow : (t + 1) * narrow], part)
        moe_part = jnp.where(place == t, moe_gain[:, t * narrow : (t + 1) * narrow], moe_part)
    slice_ref[...] = part
    moe_slice_ref[...] = jnp.broadcast_to(moe_part, moe_slice_ref.shape)

    slots = choice_ref.shape[1]
    top = routing_ref.shape[0]
    capacity = CAPACITY
    i = lax.broadcasted_iota(jnp.int32, (rows, rows), 0)
    j = lax.broadcasted_iota(jnp.int32, (rows, rows), 1)
    eye = (i == j).astype(F32)
    across = (((1,), (1,)), ((), ()))
    chosen = lax.dot_general(
        eye, routing_ref[...].astype(F32), across, precision=lax.Precision.HIGHEST, preferred_element_type=F32
    )
    weights = lax.dot_general(
        eye, weight_ref[...], across, precision=lax.Precision.HIGHEST, preferred_element_type=F32
    )
    lane = lax.broadcasted_iota(jnp.int32, (rows, slots), 1)
    expert = (lane // capacity).astype(F32)
    named = jnp.zeros((rows, slots), F32)
    weight = jnp.zeros((rows, slots), F32)
    for k in range(top):
        hit = chosen[:, k : k + 1] == expert
        named = jnp.where(hit, 1.0, named)
        weight = jnp.where(hit, weights[:, k : k + 1], weight)
    earlier = jnp.dot((j < i).astype(BF16), named.astype(BF16), preferred_element_type=F32)
    filled = (named > 0.5) & (earlier == (lane % capacity).astype(F32))
    choice_ref[...] = jnp.where(filled, 1.0, 0.0).astype(BF16)
    mix_ref[...] = jnp.where(filled, weight, 0.0)


def half_sums(normed, packed_ref, core, rows):
    lane = lax.broadcasted_iota(jnp.int32, (rows, 128), 1)
    taken = (lane // 64) == core
    total = jnp.zeros((rows, 256), F32)
    forget = jnp.zeros((rows, 128), F32)
    for z in range(packed_ref.shape[0]):
        left = normed[:, z * 128 : (z + 1) * 128]
        left = jnp.where(taken, left, jnp.zeros_like(left))
        block = packed_ref[z, :64, :]
        total = total + jnp.dot(left, jnp.concatenate([block, block], axis=0), preferred_element_type=F32)
        weights = packed_ref[z, 64:72, :128][:1, :64]
        forget = forget + left.astype(F32) * jnp.concatenate([weights, weights], axis=1).astype(F32)
    return jnp.concatenate([total, forget], axis=1)


def attention_kernel(
    core_ref, bias_ref, lengths_ref, normed_ref, sums_ref, mine_ref, theirs_ref, keys_ref, values_ref, gates_ref, out_ref
):
    rows = normed_ref.shape[0]
    cached = keys_ref.shape[1]
    head = keys_ref.shape[0] // rows
    chips = mine_ref.shape[0]
    core = core_ref[0]
    is_odd = core == 1
    own = sums_ref[...]
    other = half_sums(normed_ref[...], theirs_ref, 1 - core, rows)
    both = own + other
    query = both[:, :head].astype(BF16)
    key_new = both[:, head : 2 * head].astype(BF16)
    value_new = both[:, 2 * head : 3 * head].astype(BF16)
    forget_pre = jnp.sum(both[:, 256:], axis=1, keepdims=True) + bias_ref[0]
    log_gate = jnp.minimum(forget_pre, 0.0) - jnp.log1p(jnp.exp(-jnp.abs(forget_pre)))

    gates = gates_ref[...].reshape(rows, cached)
    row = lax.broadcasted_iota(jnp.int32, (rows, 1), 0)
    count = jnp.zeros((rows, 1), jnp.int32)
    for s in range(rows):
        count = jnp.where(row == s, lengths_ref[s], count)
    position = lax.broadcasted_iota(jnp.int32, (rows, cached), 1)
    last_gate = jnp.sum(jnp.where(position == count - 1, gates, 0.0), axis=-1, keepdims=True)
    new_gate = last_gate + log_gate

    owner = lax.broadcasted_iota(jnp.int32, (rows, rows * head), 1) // head
    diagonal = owner == lax.broadcasted_iota(jnp.int32, (rows, rows * head), 0)
    repeated = jnp.concatenate([query] * rows, axis=1)
    spread = jnp.where(diagonal, repeated, jnp.zeros_like(repeated))
    scale = head ** (-0.5)
    scores = jnp.dot(spread, keys_ref[...], preferred_element_type=F32) * scale
    scores = scores + (new_gate - gates)
    scores = jnp.where(position < count, scores, -jnp.inf)
    own_score = jnp.sum(query.astype(F32) * key_new.astype(F32), axis=-1, keepdims=True) * scale
    highest = jnp.maximum(jnp.max(scores, axis=-1, keepdims=True), own_score)
    cached_weight = jnp.exp(scores - highest)
    own_weight = jnp.exp(own_score - highest)
    denominator = jnp.sum(cached_weight, axis=-1, keepdims=True) + own_weight
    share = (cached_weight / denominator).astype(BF16)
    crossed = lax.dot_general(
        share, values_ref[...], (((1,), (1,)), ((), ())), preferred_element_type=F32
    )
    crossed = jnp.where(diagonal, crossed, 0.0)
    folded = crossed[:, :128]
    for b in range(1, rows * head // 128):
        folded = folded + crossed[:, b * 128 : (b + 1) * 128]
    attended = folded[:, :head] + folded[:, head:]
    attended = attended + (own_weight / denominator) * value_new.astype(F32)
    attended = attended.astype(BF16)
    lane = lax.broadcasted_iota(jnp.int32, (rows, 128), 1)
    for z in range(chips):
        mine = jnp.dot(attended, mine_ref[z, :64, 128:], preferred_element_type=F32)
        theirs = jnp.dot(attended, theirs_ref[z, :64, 128:], preferred_element_type=F32)
        even = jnp.where(is_odd, theirs, mine)
        odd = jnp.where(is_odd, mine, theirs)
        out_ref[z] = jnp.where(lane < head, pltpu.roll(even, head, 1), odd)


def expert_kernel(rows_ref, gain_ref, gate_ref, up_ref, down_ref, out_ref):
    tiles, slots, narrow = rows_ref.shape
    width = tiles * narrow
    inverse = 1.0 / gain_ref[...].astype(F32).reshape(1, width)
    squares = jnp.zeros((slots, narrow), F32)
    products = jnp.zeros((slots, 2 * gate_ref.shape[0]), F32)
    for t in range(tiles):
        part = rows_ref[t]
        plain = part.astype(F32) * inverse[:, t * narrow : (t + 1) * narrow]
        squares = squares + plain * plain
        weights = jnp.concatenate(
            [gate_ref[:, t * narrow : (t + 1) * narrow], up_ref[:, t * narrow : (t + 1) * narrow]], axis=0
        )
        products = products + lax.dot_general(
            part, weights, (((1,), (1,)), ((), ())), preferred_element_type=F32
        )
    row_scale = lax.rsqrt(jnp.sum(squares, axis=1, keepdims=True) / width + NORM_EPSILON)
    products = products * row_scale
    units = gate_ref.shape[0]
    gate_cut = jnp.minimum(products[:, :units], CLAMP_LIMIT)
    up_cut = jnp.clip(products[:, units:], -CLAMP_LIMIT, CLAMP_LIMIT)
    hidden = ((up_cut + 1.0) * gate_cut * jax.nn.sigmoid(SIGMOID_SLOPE * gate_cut)).astype(BF16)
    for t in range(tiles):
        part = jnp.dot(hidden, down_ref[:, t * narrow : (t + 1) * narrow], preferred_element_type=F32)
        out_ref[t] = part.astype(BF16)


def spread_kernel(parts_ref, slice_ref, moe_slice_ref, choice_ref, residual_ref, sent_ref):
    residual = slice_ref[...]
    for t in range(parts_ref.shape[0]):
        residual = residual + parts_ref[t]
    residual_ref[...] = residual
    scaled = (residual * moe_slice_ref[:1, :]).astype(BF16)
    sent_ref[...] = lax.dot_general(
        choice_ref[...], scaled, (((0,), (0,)), ((), ())), preferred_element_type=F32
    ).astype(BF16)


def gather_kernel(parts_ref, out_ref):
    total = parts_ref[0].astype(F32)
    for t in range(1, parts_ref.shape[0]):
        total = total + parts_ref[t].astype(F32)
    out_ref[...] = total.astype(BF16)


def combine_kernel(returned_ref, mix_ref, residual_ref, out_ref):
    expert_sum = jnp.dot(
        mix_ref[...],
        returned_ref[...].astype(F32),
        precision=lax.Precision.HIGHEST,
        preferred_element_type=F32,
    )
    out = (residual_ref[...] + expert_sum).astype(BF16)
    for t in range(out_ref.shape[0]):
        out_ref[t] = out


def local(
    tokens,
    attn_gain,
    w_query,
    w_key,
    w_value,
    w_forget,
    forget_bias,
    cache_keys,
    cache_values,
    cache_gates,
    lengths,
    w_out,
    moe_gain,
    routing,
    route_weight,
    w_gate,
    w_up,
    w_down,
):
    n_ep = lax.axis_size("ep")
    n_tp = lax.axis_size("tp")
    rows, width = tokens.shape
    narrow = width // n_tp
    chips = n_ep // 2
    head = cache_keys.shape[3]
    cached = cache_keys.shape[2]
    slots = n_ep * CAPACITY
    core = (lax.axis_index("ep") % 2).reshape(1)
    place = lax.axis_index("tp").reshape(1)
    smem = pl.BlockSpec(memory_space=pltpu.SMEM)
    vmem = pl.BlockSpec(memory_space=pltpu.VMEM)
    params = pltpu.CompilerParams(vmem_limit_bytes=LIMIT)

    busy = pl.CostEstimate(flops=10**9, bytes_accessed=1, transcendentals=0)

    def kernel(body, name, outs, ins, cost=None):
        return pl.pallas_call(
            body,
            out_shape=tuple(jax.ShapeDtypeStruct(*o) for o in outs),
            in_specs=ins,
            out_specs=tuple(vmem for _ in outs),
            compiler_params=params,
            cost_estimate=cost,
            name=name,
        )

    packed = jnp.concatenate([w_query, w_key, w_value, w_out], axis=1)
    forget_row = jnp.pad(w_forget.T, ((0, PACK_ROWS - 65), (0, packed.shape[1] - 64)))
    packed = jnp.concatenate([packed, forget_row], axis=0)
    (packed,) = kernel(settle_kernel, "settle", [(packed.shape, BF16)], [vmem], cost=busy)(packed)
    same_core = [[2 * z + c for z in range(chips)] for c in range(2)]
    mine = lax.all_gather(packed, "ep", axis=0, tiled=False, axis_index_groups=same_core)
    theirs = lax.ppermute(mine, "ep", [(i, i ^ 1) for i in range(n_ep)])

    normed, sums, token_slice, moe_slice, choice, mix = kernel(
        prepare_kernel,
        "prepare",
        [
            ((rows, width), BF16),
            ((rows, 384), F32),
            ((rows, narrow), F32),
            ((8, narrow), F32),
            ((rows, slots), BF16),
            ((rows, slots), F32),
        ],
        [smem, smem] + [vmem] * 6,
        cost=busy,
    )(
        core,
        place,
        mine,
        tokens,
        attn_gain,
        moe_gain,
        routing.T,
        route_weight.T,
    )
    (head_terms,) = kernel(
        attention_kernel,
        "attention",
        [((n_tp, rows, narrow), F32)],
        [smem, smem, smem] + [vmem] * 7,
        cost=busy,
    )(
        core,
        forget_bias,
        lengths,
        normed,
        sums,
        mine,
        theirs,
        jnp.swapaxes(cache_keys[:, 0], 1, 2).reshape(rows * head, cached),
        jnp.swapaxes(cache_values[:, 0], 1, 2).reshape(rows * head, cached),
        cache_gates,
    )

    parts = lax.all_to_all(head_terms, "tp", 0, 0, tiled=True)
    residual, sent = kernel(
        spread_kernel, "spread", [((rows, narrow), F32), ((slots, narrow), BF16)], [vmem] * 4
    )(parts, token_slice, moe_slice, choice)
    received = lax.all_to_all(sent.reshape(n_ep, CAPACITY, narrow), "ep", 0, 0, tiled=True)
    full = to_everyone(received.reshape(slots, narrow), "tp")
    (partial,) = kernel(expert_kernel, "experts", [((n_tp, slots, narrow), BF16)], [vmem] * 5)(
        full, moe_gain, jnp.swapaxes(w_gate[0], 0, 1), jnp.swapaxes(w_up[0], 0, 1), w_down[0]
    )
    partial = lax.all_to_all(partial, "tp", 0, 0, tiled=True)
    (served,) = kernel(gather_kernel, "served", [((slots, narrow), BF16)], [vmem])(partial)
    returned = lax.all_to_all(served.reshape(n_ep, CAPACITY, narrow), "ep", 0, 0, tiled=True)
    (copies_out,) = kernel(combine_kernel, "combine", [((n_tp, rows, narrow), BF16)], [vmem] * 3)(
        returned.reshape(slots, narrow), mix, residual
    )
    final = lax.all_to_all(copies_out, "tp", 0, 0, tiled=True)
    return jnp.moveaxis(final, 0, 1).reshape(rows, width)


def solution(mesh):
    in_specs = (
        P("ep", None),
        P(),
        P("ep", "tp"),
        P("ep", "tp"),
        P("ep", "tp"),
        P("ep", "tp"),
        P("tp"),
        P("ep", "tp", None, None),
        P("ep", "tp", None, None),
        P("ep", "tp", None),
        P("ep"),
        P("tp", "ep"),
        P(),
        P("ep", None),
        P("ep", None),
        P("ep", None, "tp"),
        P("ep", None, "tp"),
        P("ep", "tp", None),
    )
    out_specs = P("ep", None)
    return jax.shard_map(local, mesh=mesh, in_specs=in_specs, out_specs=out_specs, check_vma=False)
```

```python
import jax
import jax.numpy as jnp
from jax import lax
from jax.experimental import pallas as pl
from jax.experimental.pallas import tpu as pltpu
from jax.sharding import PartitionSpec as P

NORM_EPSILON = 1e-06
CLAMP_LIMIT = 7.0
SIGMOID_SLOPE = 1.702
F32 = jnp.float32
BF16 = jnp.bfloat16


def exchanged(tiles, axis, order):
    return lax.all_to_all(tiles, axis, 0, 0, tiled=True, axis_index_groups=[order])


PACK_ROWS = 72
LIMIT = 16 * 2**20
CAPACITY = 4
RING = list(range(16))
PLANE = [5, 2, 3, 10, 13, 0, 7, 14, 4, 8, 12, 1, 11, 6, 9, 15]
LINE = [i ^ 17 for i in range(32)]


def settle_kernel(packed_ref, out_ref):
    out_ref[...] = packed_ref[...]


def prepare_kernel(
    core_ref, place_ref, mine_ref, tokens_ref, gain_ref, moe_gain_ref, routing_ref, weight_ref,
    normed_ref, sums_ref, slice_ref, moe_slice_ref, choice_ref, mix_ref,
):
    rows, width = tokens_ref.shape
    narrow = slice_ref.shape[1]
    tokens = tokens_ref[...]
    wide = tokens.astype(F32)
    scale_row = lax.rsqrt(jnp.mean(wide * wide, axis=-1, keepdims=True) + NORM_EPSILON)
    normed = (wide * scale_row * gain_ref[...].astype(F32).reshape(1, width)).astype(BF16)
    normed_ref[...] = normed
    sums_ref[...] = half_sums(normed, mine_ref, core_ref[0], rows)

    place = place_ref[0]
    moe_gain = moe_gain_ref[...].astype(F32).reshape(1, width)
    part = jnp.zeros((rows, narrow), F32)
    moe_part = jnp.zeros((1, narrow), F32)
    for t in range(width // narrow):
        part = jnp.where(place == t, wide[:, t * narrow : (t + 1) * narrow], part)
        moe_part = jnp.where(place == t, moe_gain[:, t * narrow : (t + 1) * narrow], moe_part)
    slice_ref[...] = part
    moe_slice_ref[...] = jnp.broadcast_to(moe_part, moe_slice_ref.shape)

    slots = choice_ref.shape[1]
    top = routing_ref.shape[0]
    capacity = CAPACITY
    i = lax.broadcasted_iota(jnp.int32, (rows, rows), 0)
    j = lax.broadcasted_iota(jnp.int32, (rows, rows), 1)
    eye = (i == j).astype(F32)
    across = (((1,), (1,)), ((), ()))
    chosen = lax.dot_general(
        eye, routing_ref[...].astype(F32), across, precision=lax.Precision.HIGHEST, preferred_element_type=F32
    )
    weights = lax.dot_general(
        eye, weight_ref[...], across, precision=lax.Precision.HIGHEST, preferred_element_type=F32
    )
    lane = lax.broadcasted_iota(jnp.int32, (rows, slots), 1)
    expert = ((lane // capacity) ^ 17).astype(F32)
    named = jnp.zeros((rows, slots), F32)
    weight = jnp.zeros((rows, slots), F32)
    for k in range(top):
        hit = chosen[:, k : k + 1] == expert
        named = jnp.where(hit, 1.0, named)
        weight = jnp.where(hit, weights[:, k : k + 1], weight)
    earlier = jnp.dot((j < i).astype(BF16), named.astype(BF16), preferred_element_type=F32)
    filled = (named > 0.5) & (earlier == (lane % capacity).astype(F32))
    choice_ref[...] = jnp.where(filled, 1.0, 0.0).astype(BF16)
    mix_ref[...] = jnp.where(filled, weight, 0.0)


def half_sums(normed, packed_ref, core, rows):
    lane = lax.broadcasted_iota(jnp.int32, (rows, 128), 1)
    taken = (lane // 64) == core
    total = jnp.zeros((rows, 256), F32)
    forget = jnp.zeros((rows, 128), F32)
    for z in range(packed_ref.shape[0]):
        left = normed[:, RING[z] * 128 : (RING[z] + 1) * 128]
        left = jnp.where(taken, left, jnp.zeros_like(left))
        block = packed_ref[z, :64, :]
        total = total + jnp.dot(left, jnp.concatenate([block, block], axis=0), preferred_element_type=F32)
        weights = packed_ref[z, 64:72, :128][:1, :64]
        forget = forget + left.astype(F32) * jnp.concatenate([weights, weights], axis=1).astype(F32)
    return jnp.concatenate([total, forget], axis=1)


def attention_kernel(
    core_ref, bias_ref, lengths_ref, normed_ref, sums_ref, mine_ref, theirs_ref, keys_ref, values_ref, gates_ref, out_ref
):
    rows = normed_ref.shape[0]
    cached = keys_ref.shape[1]
    head = keys_ref.shape[0] // rows
    chips = mine_ref.shape[0]
    core = core_ref[0]
    is_odd = core == 1
    own = sums_ref[...]
    other = half_sums(normed_ref[...], theirs_ref, 1 - core, rows)
    both = own + other
    query = both[:, :head].astype(BF16)
    key_new = both[:, head : 2 * head].astype(BF16)
    value_new = both[:, 2 * head : 3 * head].astype(BF16)
    forget_pre = jnp.sum(both[:, 256:], axis=1, keepdims=True) + bias_ref[0]
    log_gate = jnp.minimum(forget_pre, 0.0) - jnp.log1p(jnp.exp(-jnp.abs(forget_pre)))

    gates = gates_ref[...].reshape(rows, cached)
    row = lax.broadcasted_iota(jnp.int32, (rows, 1), 0)
    count = jnp.zeros((rows, 1), jnp.int32)
    for s in range(rows):
        count = jnp.where(row == s, lengths_ref[s], count)
    position = lax.broadcasted_iota(jnp.int32, (rows, cached), 1)
    last_gate = jnp.sum(jnp.where(position == count - 1, gates, 0.0), axis=-1, keepdims=True)
    new_gate = last_gate + log_gate

    owner = lax.broadcasted_iota(jnp.int32, (rows, rows * head), 1) // head
    diagonal = owner == lax.broadcasted_iota(jnp.int32, (rows, rows * head), 0)
    repeated = jnp.concatenate([query] * rows, axis=1)
    spread = jnp.where(diagonal, repeated, jnp.zeros_like(repeated))
    scale = head ** (-0.5)
    scores = jnp.dot(spread, keys_ref[...], preferred_element_type=F32) * scale
    scores = scores + (new_gate - gates)
    scores = jnp.where(position < count, scores, -jnp.inf)
    own_score = jnp.sum(query.astype(F32) * key_new.astype(F32), axis=-1, keepdims=True) * scale
    highest = jnp.maximum(jnp.max(scores, axis=-1, keepdims=True), own_score)
    cached_weight = jnp.exp(scores - highest)
    own_weight = jnp.exp(own_score - highest)
    denominator = jnp.sum(cached_weight, axis=-1, keepdims=True) + own_weight
    share = (cached_weight / denominator).astype(BF16)
    crossed = lax.dot_general(
        share, values_ref[...], (((1,), (1,)), ((), ())), preferred_element_type=F32
    )
    crossed = jnp.where(diagonal, crossed, 0.0)
    folded = crossed[:, :128]
    for b in range(1, rows * head // 128):
        folded = folded + crossed[:, b * 128 : (b + 1) * 128]
    attended = folded[:, :head] + folded[:, head:]
    attended = attended + (own_weight / denominator) * value_new.astype(F32)
    attended = attended.astype(BF16)
    lane = lax.broadcasted_iota(jnp.int32, (rows, 128), 1)
    for i, chip in enumerate(PLANE):
        z = RING.index(chip)
        mine = jnp.dot(attended, mine_ref[z, :64, 128:], preferred_element_type=F32)
        theirs = jnp.dot(attended, theirs_ref[z, :64, 128:], preferred_element_type=F32)
        even = jnp.where(is_odd, theirs, mine)
        odd = jnp.where(is_odd, mine, theirs)
        out_ref[i] = jnp.where(lane < head, pltpu.roll(even, head, 1), odd)


def expert_kernel(rows_ref, gain_ref, gate_ref, up_ref, down_ref, out_ref):
    tiles, slots, narrow = rows_ref.shape
    width = tiles * narrow
    inverse = 1.0 / gain_ref[...].astype(F32).reshape(1, width)
    squares = jnp.zeros((slots, narrow), F32)
    products = jnp.zeros((slots, 2 * gate_ref.shape[0]), F32)
    for t in range(tiles):
        part = rows_ref[t]
        at = slice(PLANE[t] * narrow, (PLANE[t] + 1) * narrow)
        plain = part.astype(F32) * inverse[:, at]
        squares = squares + plain * plain
        weights = jnp.concatenate(
            [gate_ref[:, at], up_ref[:, at]], axis=0
        )
        products = products + lax.dot_general(
            part, weights, (((1,), (1,)), ((), ())), preferred_element_type=F32
        )
    row_scale = lax.rsqrt(jnp.sum(squares, axis=1, keepdims=True) / width + NORM_EPSILON)
    products = products * row_scale
    units = gate_ref.shape[0]
    gate_cut = jnp.minimum(products[:, :units], CLAMP_LIMIT)
    up_cut = jnp.clip(products[:, units:], -CLAMP_LIMIT, CLAMP_LIMIT)
    hidden = ((up_cut + 1.0) * gate_cut * jax.nn.sigmoid(SIGMOID_SLOPE * gate_cut)).astype(BF16)
    for t in range(tiles):
        at = slice(PLANE[t] * narrow, (PLANE[t] + 1) * narrow)
        part = jnp.dot(hidden, down_ref[:, at], preferred_element_type=F32)
        out_ref[t] = part.astype(BF16)


def spread_kernel(parts_ref, slice_ref, moe_slice_ref, choice_ref, residual_ref, sent_ref):
    residual = slice_ref[...]
    for t in range(parts_ref.shape[0]):
        residual = residual + parts_ref[t]
    residual_ref[...] = residual
    scaled = (residual * moe_slice_ref[:1, :]).astype(BF16)
    sent_ref[...] = lax.dot_general(
        choice_ref[...], scaled, (((0,), (0,)), ((), ())), preferred_element_type=F32
    ).astype(BF16)


def gather_kernel(parts_ref, out_ref):
    total = parts_ref[0].astype(F32)
    for t in range(1, parts_ref.shape[0]):
        total = total + parts_ref[t].astype(F32)
    out_ref[...] = total.astype(BF16)


def combine_kernel(returned_ref, mix_ref, residual_ref, out_ref):
    expert_sum = jnp.dot(
        mix_ref[...],
        returned_ref[...].astype(F32),
        precision=lax.Precision.HIGHEST,
        preferred_element_type=F32,
    )
    out = (residual_ref[...] + expert_sum).astype(BF16)
    for t in range(out_ref.shape[0]):
        out_ref[t] = out


def local(
    tokens,
    attn_gain,
    w_query,
    w_key,
    w_value,
    w_forget,
    forget_bias,
    cache_keys,
    cache_values,
    cache_gates,
    lengths,
    w_out,
    moe_gain,
    routing,
    route_weight,
    w_gate,
    w_up,
    w_down,
):
    n_ep = lax.axis_size("ep")
    n_tp = lax.axis_size("tp")
    rows, width = tokens.shape
    narrow = width // n_tp
    chips = n_ep // 2
    head = cache_keys.shape[3]
    cached = cache_keys.shape[2]
    slots = n_ep * CAPACITY
    core = (lax.axis_index("ep") % 2).reshape(1)
    place = lax.axis_index("tp").reshape(1)
    smem = pl.BlockSpec(memory_space=pltpu.SMEM)
    vmem = pl.BlockSpec(memory_space=pltpu.VMEM)
    params = pltpu.CompilerParams(vmem_limit_bytes=LIMIT)

    busy = pl.CostEstimate(flops=10**9, bytes_accessed=1, transcendentals=0)

    def kernel(body, name, outs, ins, cost=None):
        return pl.pallas_call(
            body,
            out_shape=tuple(jax.ShapeDtypeStruct(*o) for o in outs),
            in_specs=ins,
            out_specs=tuple(vmem for _ in outs),
            compiler_params=params,
            cost_estimate=cost,
            name=name,
        )

    packed = jnp.concatenate([w_query, w_key, w_value, w_out], axis=1)
    forget_row = jnp.pad(w_forget.T, ((0, PACK_ROWS - 65), (0, packed.shape[1] - 64)))
    packed = jnp.concatenate([packed, forget_row], axis=0)
    (packed,) = kernel(settle_kernel, "settle", [(packed.shape, BF16)], [vmem], cost=busy)(packed)
    same_core = [[2 * z + c for z in RING] for c in range(2)]
    mine = lax.all_gather(packed, "ep", axis=0, tiled=False, axis_index_groups=same_core)
    theirs = lax.ppermute(mine, "ep", [(i, i ^ 1) for i in range(n_ep)])

    normed, sums, token_slice, moe_slice, choice, mix = kernel(
        prepare_kernel,
        "prepare",
        [
            ((rows, width), BF16),
            ((rows, 384), F32),
            ((rows, narrow), F32),
            ((8, narrow), F32),
            ((rows, slots), BF16),
            ((rows, slots), F32),
        ],
        [smem, smem] + [vmem] * 6,
        cost=busy,
    )(
        core,
        place,
        mine,
        tokens,
        attn_gain,
        moe_gain,
        routing.T,
        route_weight.T,
    )
    (head_terms,) = kernel(
        attention_kernel,
        "attention",
        [((n_tp, rows, narrow), F32)],
        [smem, smem, smem] + [vmem] * 7,
        cost=busy,
    )(
        core,
        forget_bias,
        lengths,
        normed,
        sums,
        mine,
        theirs,
        jnp.swapaxes(cache_keys[:, 0], 1, 2).reshape(rows * head, cached),
        jnp.swapaxes(cache_values[:, 0], 1, 2).reshape(rows * head, cached),
        cache_gates,
    )

    parts = exchanged(head_terms, "tp", PLANE)
    residual, sent = kernel(
        spread_kernel, "spread", [((rows, narrow), F32), ((slots, narrow), BF16)], [vmem] * 4
    )(parts, token_slice, moe_slice, choice)
    received = exchanged(sent.reshape(n_ep, CAPACITY, narrow), "ep", LINE)
    full = jnp.broadcast_to(received.reshape(1, slots, narrow), (n_tp, slots, narrow))
    full = exchanged(full, "tp", PLANE)
    (partial,) = kernel(expert_kernel, "experts", [((n_tp, slots, narrow), BF16)], [vmem] * 5)(
        full, moe_gain, jnp.swapaxes(w_gate[0], 0, 1), jnp.swapaxes(w_up[0], 0, 1), w_down[0]
    )
    partial = exchanged(partial, "tp", PLANE)
    (served,) = kernel(gather_kernel, "served", [((slots, narrow), BF16)], [vmem])(partial)
    returned = exchanged(served.reshape(n_ep, CAPACITY, narrow), "ep", LINE)
    (copies_out,) = kernel(combine_kernel, "combine", [((n_tp, rows, narrow), BF16)], [vmem] * 3)(
        returned.reshape(slots, narrow), mix, residual
    )
    final = lax.all_to_all(copies_out, "tp", 0, 0, tiled=True)
    return jnp.moveaxis(final, 0, 1).reshape(rows, width)


def solution(mesh):
    in_specs = (
        P("ep", None),
        P(),
        P("ep", "tp"),
        P("ep", "tp"),
        P("ep", "tp"),
        P("ep", "tp"),
        P("tp"),
        P("ep", "tp", None, None),
        P("ep", "tp", None, None),
        P("ep", "tp", None),
        P("ep"),
        P("tp", "ep"),
        P(),
        P("ep", None),
        P("ep", None),
        P("ep", None, "tp"),
        P("ep", None, "tp"),
        P("ep", "tp", None),
    )
    out_specs = P("ep", None)
    return jax.shard_map(local, mesh=mesh, in_specs=in_specs, out_specs=out_specs, check_vma=False)
```

```python
import jax
import jax.numpy as jnp
from jax import lax
from jax.experimental import pallas as pl
from jax.experimental.pallas import tpu as pltpu
from jax.sharding import PartitionSpec as P

NORM_EPSILON = 1e-06
CLAMP_LIMIT = 7.0
SIGMOID_SLOPE = 1.702
F32 = jnp.float32
BF16 = jnp.bfloat16


def exchanged(tiles, axis, order):
    return lax.all_to_all(tiles, axis, 0, 0, tiled=True, axis_index_groups=[order])


PACK_ROWS = 72
LIMIT = 16 * 2**20
CAPACITY = 4
RING = list(range(16))
PLANE = [5, 2, 3, 10, 13, 0, 7, 14, 4, 8, 12, 1, 11, 6, 9, 15]
LINE = [i ^ 17 for i in range(32)]


def settle_kernel(packed_ref, out_ref):
    out_ref[...] = packed_ref[...]


def prepare_kernel(
    core_ref, place_ref, mine_ref, tokens_ref, gain_ref, moe_gain_ref, routing_ref, weight_ref,
    normed_ref, sums_ref, slice_ref, moe_slice_ref, choice_ref, mix_ref,
):
    rows, width = tokens_ref.shape
    narrow = slice_ref.shape[1]
    tokens = tokens_ref[...]
    wide = tokens.astype(F32)
    scale_row = lax.rsqrt(jnp.mean(wide * wide, axis=-1, keepdims=True) + NORM_EPSILON)
    normed = (wide * scale_row * gain_ref[...].astype(F32).reshape(1, width)).astype(BF16)
    normed_ref[...] = normed
    sums_ref[...] = half_sums(normed, mine_ref, core_ref[0], rows)

    place = place_ref[0]
    moe_gain = moe_gain_ref[...].astype(F32).reshape(1, width)
    part = jnp.zeros((rows, narrow), F32)
    moe_part = jnp.zeros((1, narrow), F32)
    for t in range(width // narrow):
        part = jnp.where(place == t, wide[:, t * narrow : (t + 1) * narrow], part)
        moe_part = jnp.where(place == t, moe_gain[:, t * narrow : (t + 1) * narrow], moe_part)
    slice_ref[...] = part
    moe_slice_ref[...] = jnp.broadcast_to(moe_part, moe_slice_ref.shape)

    slots = choice_ref.shape[1]
    top = routing_ref.shape[0]
    capacity = CAPACITY
    i = lax.broadcasted_iota(jnp.int32, (rows, rows), 0)
    j = lax.broadcasted_iota(jnp.int32, (rows, rows), 1)
    eye = (i == j).astype(F32)
    across = (((1,), (1,)), ((), ()))
    chosen = lax.dot_general(
        eye, routing_ref[...].astype(F32), across, precision=lax.Precision.HIGHEST, preferred_element_type=F32
    )
    weights = lax.dot_general(
        eye, weight_ref[...], across, precision=lax.Precision.HIGHEST, preferred_element_type=F32
    )
    lane = lax.broadcasted_iota(jnp.int32, (rows, slots), 1)
    expert = ((lane // capacity) ^ 17).astype(F32)
    named = jnp.zeros((rows, slots), F32)
    weight = jnp.zeros((rows, slots), F32)
    for k in range(top):
        hit = chosen[:, k : k + 1] == expert
        named = jnp.where(hit, 1.0, named)
        weight = jnp.where(hit, weights[:, k : k + 1], weight)
    earlier = jnp.dot((j < i).astype(BF16), named.astype(BF16), preferred_element_type=F32)
    filled = (named > 0.5) & (earlier == (lane % capacity).astype(F32))
    choice_ref[...] = jnp.where(filled, 1.0, 0.0).astype(BF16)
    mix_ref[...] = jnp.where(filled, weight, 0.0)


def half_sums(normed, packed_ref, core, rows):
    lane = lax.broadcasted_iota(jnp.int32, (rows, 128), 1)
    taken = (lane // 64) == core
    total = jnp.zeros((rows, 256), F32)
    forget = jnp.zeros((rows, 128), F32)
    for z in range(packed_ref.shape[0]):
        left = normed[:, RING[z] * 128 : (RING[z] + 1) * 128]
        left = jnp.where(taken, left, jnp.zeros_like(left))
        block = packed_ref[z, :64, :]
        total = total + jnp.dot(left, jnp.concatenate([block, block], axis=0), preferred_element_type=F32)
        weights = packed_ref[z, 64:72, :128][:1, :64]
        forget = forget + left.astype(F32) * jnp.concatenate([weights, weights], axis=1).astype(F32)
    return jnp.concatenate([total, forget], axis=1)


def attention_kernel(
    core_ref, bias_ref, lengths_ref, normed_ref, sums_ref, mine_ref, theirs_ref, keys_ref, values_ref, gates_ref, out_ref
):
    rows = normed_ref.shape[0]
    cached = keys_ref.shape[1]
    head = keys_ref.shape[0] // rows
    chips = mine_ref.shape[0]
    core = core_ref[0]
    is_odd = core == 1
    own = sums_ref[...]
    other = half_sums(normed_ref[...], theirs_ref, 1 - core, rows)
    both = own + other
    query = both[:, :head].astype(BF16)
    key_new = both[:, head : 2 * head].astype(BF16)
    value_new = both[:, 2 * head : 3 * head].astype(BF16)
    forget_pre = jnp.sum(both[:, 256:], axis=1, keepdims=True) + bias_ref[0]
    log_gate = jnp.minimum(forget_pre, 0.0) - jnp.log1p(jnp.exp(-jnp.abs(forget_pre)))

    gates = gates_ref[...].reshape(rows, cached)
    row = lax.broadcasted_iota(jnp.int32, (rows, 1), 0)
    count = jnp.zeros((rows, 1), jnp.int32)
    for s in range(rows):
        count = jnp.where(row == s, lengths_ref[s], count)
    position = lax.broadcasted_iota(jnp.int32, (rows, cached), 1)
    last_gate = jnp.sum(jnp.where(position == count - 1, gates, 0.0), axis=-1, keepdims=True)
    new_gate = last_gate + log_gate

    owner = lax.broadcasted_iota(jnp.int32, (rows, rows * head), 1) // head
    diagonal = owner == lax.broadcasted_iota(jnp.int32, (rows, rows * head), 0)
    repeated = jnp.concatenate([query] * rows, axis=1)
    spread = jnp.where(diagonal, repeated, jnp.zeros_like(repeated))
    scale = head ** (-0.5)
    scores = jnp.dot(spread, keys_ref[...], preferred_element_type=F32) * scale
    scores = scores + (new_gate - gates)
    scores = jnp.where(position < count, scores, -jnp.inf)
    own_score = jnp.sum(query.astype(F32) * key_new.astype(F32), axis=-1, keepdims=True) * scale
    highest = jnp.maximum(jnp.max(scores, axis=-1, keepdims=True), own_score)
    cached_weight = jnp.exp(scores - highest)
    own_weight = jnp.exp(own_score - highest)
    denominator = jnp.sum(cached_weight, axis=-1, keepdims=True) + own_weight
    share = (cached_weight / denominator).astype(BF16)
    crossed = lax.dot_general(
        share, values_ref[...], (((1,), (1,)), ((), ())), preferred_element_type=F32
    )
    crossed = jnp.where(diagonal, crossed, 0.0)
    folded = crossed[:, :128]
    for b in range(1, rows * head // 128):
        folded = folded + crossed[:, b * 128 : (b + 1) * 128]
    attended = folded[:, :head] + folded[:, head:]
    attended = attended + (own_weight / denominator) * value_new.astype(F32)
    attended = attended.astype(BF16)
    lane = lax.broadcasted_iota(jnp.int32, (rows, 128), 1)
    for i, chip in enumerate(PLANE):
        z = RING.index(chip)
        mine = jnp.dot(attended, mine_ref[z, :64, 128:], preferred_element_type=F32)
        theirs = jnp.dot(attended, theirs_ref[z, :64, 128:], preferred_element_type=F32)
        even = jnp.where(is_odd, theirs, mine)
        odd = jnp.where(is_odd, mine, theirs)
        out_ref[i] = jnp.where(lane < head, pltpu.roll(even, head, 1), odd).astype(BF16)


def expert_kernel(rows_ref, gain_ref, gate_ref, up_ref, down_ref, out_ref):
    tiles, slots, narrow = rows_ref.shape
    width = tiles * narrow
    inverse = 1.0 / gain_ref[...].astype(F32).reshape(1, width)
    squares = jnp.zeros((slots, narrow), F32)
    products = jnp.zeros((slots, 2 * gate_ref.shape[0]), F32)
    for t in range(tiles):
        part = rows_ref[t]
        at = slice(PLANE[t] * narrow, (PLANE[t] + 1) * narrow)
        plain = part.astype(F32) * inverse[:, at]
        squares = squares + plain * plain
        weights = jnp.concatenate(
            [gate_ref[:, at], up_ref[:, at]], axis=0
        )
        products = products + lax.dot_general(
            part, weights, (((1,), (1,)), ((), ())), preferred_element_type=F32
        )
    row_scale = lax.rsqrt(jnp.sum(squares, axis=1, keepdims=True) / width + NORM_EPSILON)
    products = products * row_scale
    units = gate_ref.shape[0]
    gate_cut = jnp.minimum(products[:, :units], CLAMP_LIMIT)
    up_cut = jnp.clip(products[:, units:], -CLAMP_LIMIT, CLAMP_LIMIT)
    hidden = ((up_cut + 1.0) * gate_cut * jax.nn.sigmoid(SIGMOID_SLOPE * gate_cut)).astype(BF16)
    for t in range(tiles):
        at = slice(PLANE[t] * narrow, (PLANE[t] + 1) * narrow)
        part = jnp.dot(hidden, down_ref[:, at], preferred_element_type=F32)
        out_ref[t] = part.astype(BF16)


def spread_kernel(parts_ref, slice_ref, moe_slice_ref, choice_ref, residual_ref, sent_ref):
    residual = slice_ref[...]
    for t in range(parts_ref.shape[0]):
        residual = residual + parts_ref[t].astype(F32)
    residual_ref[...] = residual
    scaled = (residual * moe_slice_ref[:1, :]).astype(BF16)
    sent_ref[...] = lax.dot_general(
        choice_ref[...], scaled, (((0,), (0,)), ((), ())), preferred_element_type=F32
    ).astype(BF16)


def gather_kernel(parts_ref, out_ref):
    total = parts_ref[0].astype(F32)
    for t in range(1, parts_ref.shape[0]):
        total = total + parts_ref[t].astype(F32)
    out_ref[...] = total.astype(BF16)


def combine_kernel(returned_ref, mix_ref, residual_ref, out_ref):
    expert_sum = jnp.dot(
        mix_ref[...],
        returned_ref[...].astype(F32),
        precision=lax.Precision.HIGHEST,
        preferred_element_type=F32,
    )
    out = (residual_ref[...] + expert_sum).astype(BF16)
    for t in range(out_ref.shape[0]):
        out_ref[t] = out


def local(
    tokens,
    attn_gain,
    w_query,
    w_key,
    w_value,
    w_forget,
    forget_bias,
    cache_keys,
    cache_values,
    cache_gates,
    lengths,
    w_out,
    moe_gain,
    routing,
    route_weight,
    w_gate,
    w_up,
    w_down,
):
    n_ep = lax.axis_size("ep")
    n_tp = lax.axis_size("tp")
    rows, width = tokens.shape
    narrow = width // n_tp
    chips = n_ep // 2
    head = cache_keys.shape[3]
    cached = cache_keys.shape[2]
    slots = n_ep * CAPACITY
    core = (lax.axis_index("ep") % 2).reshape(1)
    place = lax.axis_index("tp").reshape(1)
    smem = pl.BlockSpec(memory_space=pltpu.SMEM)
    vmem = pl.BlockSpec(memory_space=pltpu.VMEM)
    params = pltpu.CompilerParams(vmem_limit_bytes=LIMIT)

    busy = pl.CostEstimate(flops=10**9, bytes_accessed=1, transcendentals=0)

    def kernel(body, name, outs, ins, cost=None):
        return pl.pallas_call(
            body,
            out_shape=tuple(jax.ShapeDtypeStruct(*o) for o in outs),
            in_specs=ins,
            out_specs=tuple(vmem for _ in outs),
            compiler_params=params,
            cost_estimate=cost,
            name=name,
        )

    packed = jnp.concatenate([w_query, w_key, w_value, w_out], axis=1)
    forget_row = jnp.pad(w_forget.T, ((0, PACK_ROWS - 65), (0, packed.shape[1] - 64)))
    packed = jnp.concatenate([packed, forget_row], axis=0)
    (packed,) = kernel(settle_kernel, "settle", [(packed.shape, BF16)], [vmem], cost=busy)(packed)
    same_core = [[2 * z + c for z in RING] for c in range(2)]
    mine = lax.all_gather(packed, "ep", axis=0, tiled=False, axis_index_groups=same_core)
    theirs = lax.ppermute(mine, "ep", [(i, i ^ 1) for i in range(n_ep)])

    normed, sums, token_slice, moe_slice, choice, mix = kernel(
        prepare_kernel,
        "prepare",
        [
            ((rows, width), BF16),
            ((rows, 384), F32),
            ((rows, narrow), F32),
            ((8, narrow), F32),
            ((rows, slots), BF16),
            ((rows, slots), F32),
        ],
        [smem, smem] + [vmem] * 6,
        cost=busy,
    )(
        core,
        place,
        mine,
        tokens,
        attn_gain,
        moe_gain,
        routing.T,
        route_weight.T,
    )
    (head_terms,) = kernel(
        attention_kernel,
        "attention",
        [((n_tp, rows, narrow), BF16)],
        [smem, smem, smem] + [vmem] * 7,
        cost=busy,
    )(
        core,
        forget_bias,
        lengths,
        normed,
        sums,
        mine,
        theirs,
        jnp.swapaxes(cache_keys[:, 0], 1, 2).reshape(rows * head, cached),
        jnp.swapaxes(cache_values[:, 0], 1, 2).reshape(rows * head, cached),
        cache_gates,
    )

    parts = exchanged(head_terms, "tp", PLANE)
    residual, sent = kernel(
        spread_kernel, "spread", [((rows, narrow), F32), ((slots, narrow), BF16)], [vmem] * 4
    )(parts, token_slice, moe_slice, choice)
    received = exchanged(sent.reshape(n_ep, CAPACITY, narrow), "ep", LINE)
    full = jnp.broadcast_to(received.reshape(1, slots, narrow), (n_tp, slots, narrow))
    full = exchanged(full, "tp", PLANE)
    (partial,) = kernel(expert_kernel, "experts", [((n_tp, slots, narrow), BF16)], [vmem] * 5)(
        full, moe_gain, jnp.swapaxes(w_gate[0], 0, 1), jnp.swapaxes(w_up[0], 0, 1), w_down[0]
    )
    partial = exchanged(partial, "tp", PLANE)
    (served,) = kernel(gather_kernel, "served", [((slots, narrow), BF16)], [vmem])(partial)
    returned = exchanged(served.reshape(n_ep, CAPACITY, narrow), "ep", LINE)
    (copies_out,) = kernel(combine_kernel, "combine", [((n_tp, rows, narrow), BF16)], [vmem] * 3)(
        returned.reshape(slots, narrow), mix, residual
    )
    final = lax.all_to_all(copies_out, "tp", 0, 0, tiled=True)
    return jnp.moveaxis(final, 0, 1).reshape(rows, width)


def solution(mesh):
    in_specs = (
        P("ep", None),
        P(),
        P("ep", "tp"),
        P("ep", "tp"),
        P("ep", "tp"),
        P("ep", "tp"),
        P("tp"),
        P("ep", "tp", None, None),
        P("ep", "tp", None, None),
        P("ep", "tp", None),
        P("ep"),
        P("tp", "ep"),
        P(),
        P("ep", None),
        P("ep", None),
        P("ep", None, "tp"),
        P("ep", None, "tp"),
        P("ep", "tp", None),
    )
    out_specs = P("ep", None)
    return jax.shard_map(local, mesh=mesh, in_specs=in_specs, out_specs=out_specs, check_vma=False)
```
